32 devices in a mesh: sp: 4 (over y, x), tp: 8 (over z, core).
Axes of the slice: x: 2, y: 2, z: 4, core: 2. Of those that a mesh axis runs over, the one named last changes fastest.
Arguments:
- inputs: bfloat16 [2, 2048, 4096], P(None, 'sp', 'tp'), may hold values from -16 to 16
- in_gain: float32 [4096], replicated, may hold values from 0.1 to 1.9
- key_weight: bfloat16 [4096, 2048], P(None, 'tp'), may hold values from -0.0014648438 to 0.0014648438
- value_weight: bfloat16 [4096, 4096], P(None, 'tp'), may hold values from -0.09375 to 0.09375
- decay_down: bfloat16 [4096, 32], replicated, may hold values from -0.09375 to 0.09375
- decay_up: bfloat16 [32, 2048], replicated, may hold values from -1 to 1
- decay_bias: float32 [2048], replicated, may hold values from 0 to 10
- new_query: bfloat16 [2, 2048], P(None, 'tp'), may hold values from -6 to 6
- out_gain: float32 [256], replicated, may hold values from 0.1 to 1.9
Outputs:
- cache: bfloat16 [2, 16, 128, 256], P(None, 'tp', 'sp')
- read: bfloat16 [2, 4096], P(None, 'tp')
The draws below stay inside these ranges and needn't reach their ends.
All inputs are finite; a program needn't handle non-finite values.
Results may differ from the reference program's by a relative error of at most 0.0085.
Values may be sent and summed in bfloat16 or wider, within the bound.
A program may use at most 64 MiB of HBM per device.

```python
import jax
import jax.numpy as jnp
from jax import lax

D = 4096
HEADS = 16
DK = 128
DV = 256
RANK = 32
SEQS = 2
SPAN_DEV = 512
SEQ_LEN = 2048


def draw_inputs(key, part):
    jitter_key, shared_key, level_key = jax.random.split(key, 3)
    run_length = max(SPAN_DEV // 2, 1)
    run_count = SEQ_LEN // run_length
    jitter = jax.random.normal(jitter_key, (SEQS, SEQ_LEN, D), jnp.float32)
    levels = jax.random.uniform(level_key, (16,), jnp.float32, -1.1, 1.1)
    shared = jax.random.normal(shared_key, (SEQS, run_count, D), jnp.float32)
    shared = jnp.repeat(shared, run_length, axis=1)
    factor = jnp.repeat(jnp.exp(levels), D // 16)
    return jnp.clip((jitter + 0.5 * shared) * factor, -16.0, 16.0).astype(jnp.bfloat16)


def draw_decay_bias(key, part):
    pick_key, slow_key, quick_key = jax.random.split(key, 3)
    share_slow = 0.5
    chosen = jax.random.uniform(pick_key, (HEADS * DK,), jnp.float32) < share_slow
    slow_bias = jax.random.uniform(slow_key, (HEADS * DK,), jnp.float32, 5.5, 7.0)
    quick_bias = jax.random.uniform(quick_key, (HEADS * DK,), jnp.float32, 0.0, 1.5)
    return jnp.where(chosen, slow_bias, quick_bias)


def block_levels(stream_key, dims, pieces, least, top_value):
    gain = 1.0
    for position, shards_of in pieces:
        heights = jax.random.uniform(jax.random.fold_in(jax.random.fold_in(stream_key, 6), position), (shards_of,), jnp.float32, least / len(pieces), top_value / len(pieces))
        gain = gain * jnp.repeat(jnp.exp(heights), dims[position] // shards_of).reshape((-1,) + (1,) * (len(dims) - 1 - position))
    return gain


def gaussian(stream_key, dims, scale, bound, pieces=(), held_as=jnp.bfloat16):
    result = jax.random.normal(stream_key, dims, jnp.float32) * scale
    if len(pieces) > 0:
        result = block_levels(stream_key, dims, pieces, -0.22, 0.18) * result
    return jnp.clip(result, min=-bound, max=bound).astype(held_as)


def setup_inputs(seed: int = 0) -> dict:
    arg_keys = jax.random.split(jax.random.key(seed), 10)
    inputs = draw_inputs(jax.random.fold_in(arg_keys[9], 71), 0)
    in_gain = jnp.clip(1.0 + 0.18 * jax.random.normal(arg_keys[1], (D,), jnp.float32), 0.1, 1.9)
    key_weight = gaussian(arg_keys[2], (D, HEADS * DK), (D * 4096) ** -0.5, 0.0014648438, ((1, 8),))
    value_weight = gaussian(arg_keys[3], (D, HEADS * DV), D ** -0.5, 0.09375, ((1, 8),))
    decay_down = gaussian(arg_keys[4], (D, RANK), D ** -0.5, 0.09375)
    decay_up = gaussian(arg_keys[5], (RANK, HEADS * DK), RANK ** -0.5, 1.0)
    decay_bias = draw_decay_bias(jax.random.fold_in(arg_keys[9], 71), 0)
    new_query = gaussian(arg_keys[7], (SEQS, HEADS * DK), 1.0, 6.0, ((1, 8),))
    out_gain = jnp.clip(1.0 + 0.18 * jax.random.normal(arg_keys[8], (DV,), jnp.float32), 0.1, 1.9)
    return dict(inputs=inputs, in_gain=in_gain, key_weight=key_weight, value_weight=value_weight, decay_down=decay_down, decay_up=decay_up, decay_bias=decay_bias, new_query=new_query, out_gain=out_gain)


def reference(inputs, in_gain, key_weight, value_weight, decay_down, decay_up, decay_bias, new_query, out_gain):
    scaled = (inputs * in_gain).astype(jnp.bfloat16)
    widened = inputs.astype(jnp.float32)
    inv_rms = lax.rsqrt(lax.optimization_barrier(jnp.mean(widened * widened, axis=-1)) + 1e-06).reshape(-1, 1)
    flat_rows = scaled.reshape(-1, D)
    key_rows = (jnp.dot(flat_rows, key_weight, preferred_element_type=jnp.float32) * inv_rms).astype(jnp.bfloat16)
    value_rows = (jnp.dot(flat_rows, value_weight, preferred_element_type=jnp.float32) * inv_rms).astype(jnp.bfloat16)
    low_rank = jnp.dot(flat_rows, decay_down, preferred_element_type=jnp.float32) * inv_rms
    gate_pre = jnp.dot(low_rank, decay_up.astype(jnp.float32), precision=lax.Precision.HIGHEST) + decay_bias
    log_decay = jax.nn.log_sigmoid(gate_pre) / 16.0
    block_count = SEQ_LEN // SPAN_DEV
    log_decay = log_decay.reshape(SEQS, block_count, SPAN_DEV, HEADS, DK)
    inclusive = jnp.cumsum(log_decay, axis=2)
    block_total = inclusive[:, :, -1]
    suffix = block_total[:, :, None] - inclusive
    weighted = (key_rows.reshape(SEQS, block_count, SPAN_DEV, HEADS, DK).astype(jnp.float32) * jnp.exp(suffix)).astype(jnp.bfloat16)
    block_state = jnp.einsum('sbthk,sbthv->sbhkv', weighted.astype(jnp.float32), value_rows.reshape(SEQS, block_count, SPAN_DEV, HEADS, DV).astype(jnp.float32))
    running = jnp.cumsum(block_total, axis=1)
    later_sum = running[:, -1:] - running
    state = jnp.einsum('sbhk,sbhkv->shkv', jnp.exp(later_sum), block_state)
    cache = state.astype(jnp.bfloat16)
    readout = jnp.einsum('shk,shkv->shv', new_query.reshape(SEQS, HEADS, DK).astype(jnp.float32), cache.astype(jnp.float32))
    normed = readout * lax.rsqrt(lax.optimization_barrier(jnp.mean(readout * readout, axis=-1, keepdims=True)) + 1e-06) * out_gain
    return (cache, normed.astype(jnp.bfloat16).reshape(SEQS, HEADS * DV))
```

```python
import functools

import jax
import jax.numpy as jnp
from jax import lax
from jax.experimental import pallas as pl
from jax.experimental.pallas import tpu as pltpu
from jax.sharding import PartitionSpec as P

DK = 128
DV = 256
CHUNK = 256
AHEAD = 2
MESH = pl.DeviceIdType.MESH
F32 = jnp.float32
BF16 = jnp.bfloat16


def split3(value):
    high = value.astype(BF16)
    rest = value - high.astype(F32)
    middle = rest.astype(BF16)
    low = (rest - middle.astype(F32)).astype(BF16)
    return high, middle, low


def kernel(
    n_sp,
    n_z,
    x_ref,
    gain_ref,
    wk_hbm,
    wv_hbm,
    wd_hbm,
    up_hbm,
    bias_hbm,
    query_ref,
    out_gain_ref,
    cache_ref,
    read_ref,
    xbuf,
    wk,
    wv,
    wd,
    up,
    bias,
    acc_k,
    acc_v,
    acc_l,
    acc_s,
    state,
    carry,
    tots,
    terms,
    landed,
    reads,
    load_sem,
    own_sem,
    line_send,
    pair_send,
    recv,
    tot_send,
    tot_recv,
    term_send,
    term_recv,
    read_send,
    read_recv,
):
    seqs, span, feats = x_ref.shape
    per_seq = span // CHUNK
    chunks = seqs * per_seq
    heads = wk_hbm.shape[1] // DK
    share = DK // n_sp
    model = n_z * 2 * feats
    sp = lax.axis_index("sp")
    tp = lax.axis_index("tp")
    z = tp // 2
    c = lax.rem(tp, 2)
    key_cols = heads * DK

    first = pl.multiple_of(tp * key_cols, key_cols)
    loads = [
        pltpu.make_async_copy(wk_hbm, wk, load_sem.at[0]),
        pltpu.make_async_copy(wv_hbm, wv, load_sem.at[1]),
        pltpu.make_async_copy(wd_hbm, wd, load_sem.at[2]),
        pltpu.make_async_copy(up_hbm.at[:, pl.ds(first, key_cols)], up, load_sem.at[3]),
        pltpu.make_async_copy(bias_hbm.at[:, pl.ds(first, key_cols)], bias, load_sem.at[4]),
    ]

    def chunk_rows(j):
        seq = j // per_seq
        start = (per_seq - 1 - lax.rem(j, per_seq)) * CHUNK
        return seq, pl.multiple_of(start, CHUNK)

    def own_copy(j):
        seq, start = chunk_rows(j)
        return pltpu.make_async_copy(
            x_ref.at[seq, pl.ds(start, CHUNK), :], xbuf.at[j, z, c], own_sem.at[j]
        )

    def line_copy(j, zz, way):
        return pltpu.make_async_remote_copy(
            src_ref=xbuf.at[j, zz, c],
            dst_ref=xbuf.at[j, zz, c],
            send_sem=line_send.at[(way + 1) // 2, j, zz],
            recv_sem=recv.at[j, zz, c],
            device_id={"tp": tp + 2 * way},
            device_id_type=MESH,
        )

    def pair_copy(j, zz, cc):
        return pltpu.make_async_remote_copy(
            src_ref=xbuf.at[j, zz, cc],
            dst_ref=xbuf.at[j, zz, cc],
            send_sem=pair_send.at[j, zz],
            recv_sem=recv.at[j, zz, cc],
            device_id={"tp": tp + 1 - 2 * c},
            device_id_type=MESH,
        )

    for j in range(chunks):
        own_copy(j).start()

    barrier = pltpu.get_barrier_semaphore()
    for way in (-1, 1):
        there = z + way

        @pl.when((there >= 0) & (there < n_z))
        def _():
            pl.semaphore_signal(
                barrier, inc=1, device_id={"tp": tp + 2 * way}, device_id_type=MESH
            )

    pl.semaphore_signal(barrier, inc=1, device_id={"tp": tp + 1 - 2 * c}, device_id_type=MESH)
    for off in range(1, n_sp):
        pl.semaphore_signal(
            barrier, inc=1, device_id={"sp": lax.rem(sp + off, n_sp)}, device_id_type=MESH
        )
    lines = jnp.where(z > 0, 1, 0) + jnp.where(z < n_z - 1, 1, 0)
    pl.semaphore_wait(barrier, lines + n_sp)

    def send_own(j):
        own_copy(j).wait()
        for way in (-1, 1):
            there = z + way

            @pl.when((there >= 0) & (there < n_z))
            def _():
                line_copy(j, z, way).start()

        pair_copy(j, z, c).start()

    for j in range(min(AHEAD, chunks)):
        send_own(j)
    for load in loads:
        load.start()
    for load in loads:
        load.wait()

    def clear_chunk():
        acc_k[...] = jnp.zeros_like(acc_k)
        acc_v[...] = jnp.zeros_like(acc_v)
        acc_l[...] = jnp.zeros_like(acc_l)
        acc_s[...] = jnp.zeros_like(acc_s)

    def add_shard(j, zz, cc):
        slot = zz * 2 + cc
        wide = xbuf[j, zz, cc].astype(F32)
        scaled = (wide * gain_ref[slot]).astype(BF16)
        rows = pl.ds(pl.multiple_of(slot * feats, feats), feats)
        acc_k[...] += jnp.dot(scaled, wk[rows, :], preferred_element_type=F32)
        acc_v[...] += jnp.dot(scaled, wv[rows, :], preferred_element_type=F32)
        acc_l[...] += jnp.dot(scaled, wd[rows, :], preferred_element_type=F32)
        square = wide * wide
        total = square[:, 0:128]
        for lane in range(128, feats, 128):
            total = total + square[:, lane : lane + 128]
        acc_s[...] += total

    def gather_step(j, i):
        away = (i + 1) // 2
        way = 1 - 2 * lax.rem(i, 2)
        zz = z + way * away

        @pl.when((zz >= 0) & (zz < n_z))
        def _():
            @pl.when(i > 0)
            def _():
                line_copy(j, zz, 1).wait_recv()
                onward = z - way

                @pl.when((onward >= 0) & (onward < n_z))
                def _():
                    line_copy(j, zz, -way).start()

                pair_copy(j, zz, c).start()

            add_shard(j, zz, c)
            pair_copy(j, zz, 1 - c).wait_recv()
            add_shard(j, zz, 1 - c)

    def finish_chunk(j):
        seq = j // per_seq

        @pl.when(lax.rem(j, per_seq) == 0)
        def _():
            carry[...] = jnp.zeros_like(carry)
            state[seq] = jnp.zeros(state.shape[1:], F32)

        inv_rms = lax.rsqrt(jnp.sum(acc_s[...], axis=1, keepdims=True) / model + 1e-06)
        low_rank = acc_l[...] * inv_rms
        gate = (
            jnp.dot(
                low_rank,
                up[...].astype(F32),
                precision=lax.Precision.HIGHEST,
                preferred_element_type=F32,
            )
            + bias[...]
        )
        log_decay = (jnp.minimum(gate, 0.0) - jnp.log1p(jnp.exp(-jnp.abs(gate)))) / 16.0
        later = (
            lax.broadcasted_iota(jnp.int32, (CHUNK, CHUNK), 1)
            > lax.broadcasted_iota(jnp.int32, (CHUNK, CHUNK), 0)
        ).astype(BF16)
        suffix = carry[...]
        for piece in split3(log_decay):
            suffix = suffix + jnp.dot(later, piece, preferred_element_type=F32)
        carry[...] = carry[...] + jnp.sum(log_decay, axis=0, keepdims=True)
        keys = (acc_k[...] * inv_rms).astype(BF16).astype(F32)
        weighted = keys * jnp.exp(suffix)
        values = (acc_v[...] * inv_rms).astype(BF16)
        for h in range(heads):
            part = weighted[:, h * DK : (h + 1) * DK].T.astype(BF16)
            rows = pl.ds(h * DK, DK)
            state[seq, rows, :] = state[seq, rows, :] + jnp.dot(
                part, values[:, h * DV : (h + 1) * DV], preferred_element_type=F32
            )

    peers = [lax.rem(sp + off, n_sp) for off in range(1, n_sp)]

    def tot_copy(seq, peer, slot):
        return pltpu.make_async_remote_copy(
            src_ref=tots.at[seq, sp],
            dst_ref=tots.at[seq, slot],
            send_sem=tot_send.at[seq, peer],
            recv_sem=tot_recv.at[seq, slot],
            device_id={"sp": peer},
            device_id_type=MESH,
        )

    def term_copy(seq, peer, slot):
        return pltpu.make_async_remote_copy(
            src_ref=terms.at[seq, peer],
            dst_ref=landed.at[seq, slot],
            send_sem=term_send.at[seq, peer],
            recv_sem=term_recv.at[seq, slot],
            device_id={"sp": peer},
            device_id_type=MESH,
        )

    def read_copy(seq, peer, slot):
        return pltpu.make_async_remote_copy(
            src_ref=reads.at[seq, sp],
            dst_ref=reads.at[seq, slot],
            send_sem=read_send.at[seq, peer],
            recv_sem=read_recv.at[seq, slot],
            device_id={"sp": peer},
            device_id_type=MESH,
        )

    def send_total(seq):
        tots[seq, sp] = carry[...]
        for peer in peers:
            tot_copy(seq, peer, sp).start()

    def send_terms(seq):
        for peer in peers:
            tot_copy(seq, peer, peer).wait_recv()
        after = jnp.zeros((1, key_cols), F32)
        for p in range(n_sp):
            after = after + jnp.where(p > sp, tots[seq, p], 0.0)
        factor = jnp.broadcast_to(jnp.exp(after), (128, key_cols)).T
        for h in range(heads):
            for p in range(n_sp):
                row = h * DK + p * share
                scale = factor[row : row + share, :]
                for lane in range(0, DV, 128):
                    terms[seq, p, h, :, lane : lane + 128] = (
                        state[seq, row : row + share, lane : lane + 128] * scale
                    )
        for peer in peers:
            term_copy(seq, peer, sp).start()

    def send_reads(seq):
        total = terms[seq, sp]
        for peer in peers:
            term_copy(seq, peer, peer).wait_recv()
            total = total + landed[seq, peer]
        cache = total.astype(BF16)
        cache_ref[seq] = cache
        wide = cache.astype(F32)
        chosen = (
            lax.broadcasted_iota(jnp.int32, (share, DK), 0) + sp * share
            == lax.broadcasted_iota(jnp.int32, (share, DK), 1)
        )
        for h in range(heads):
            queries = query_ref[seq : seq + 1, h * DK : (h + 1) * DK].astype(F32)
            column = jnp.sum(jnp.where(chosen, queries, 0.0), axis=1, keepdims=True)
            reads[seq, sp, h : h + 1, :] = jnp.sum(column * wide[h], axis=0, keepdims=True)
        for peer in peers:
            read_copy(seq, peer, sp).start()

    def give_read(seq):
        for peer in peers:
            read_copy(seq, peer, peer).wait_recv()
        readout = reads[seq, 0]
        for p in range(1, n_sp):
            readout = readout + reads[seq, p]
        mean = jnp.mean(readout * readout, axis=-1, keepdims=True)
        normed = (readout * lax.rsqrt(mean + 1e-06) * out_gain_ref[...]).astype(BF16)
        for h in range(heads):
            read_ref[seq : seq + 1, h * DV : (h + 1) * DV] = normed[h : h + 1, :]

    def chunk_step(j, _):
        @pl.when(j + AHEAD < chunks)
        def _():
            send_own(j + AHEAD)

        clear_chunk()

        def inner(i, _):
            gather_step(j, i)
            return 0

        lax.fori_loop(0, 2 * n_z - 1, inner, 0)
        finish_chunk(j)
        for seq in range(seqs):
            done = (seq + 1) * per_seq - 1

            @pl.when(j == done)
            def _():
                send_total(seq)

            if seq < seqs - 1:

                @pl.when(j == done + 1)
                def _():
                    send_terms(seq)

        return 0

    lax.fori_loop(0, chunks, chunk_step, 0)
    for seq in range(seqs - 1):
        send_reads(seq)
    send_terms(seqs - 1)
    send_reads(seqs - 1)
    for seq in range(seqs):
        give_read(seq)

    def drain(j, _):
        pair_copy(j, z, c).wait_send()
        for way in (-1, 1):
            there = z + way

            @pl.when((there >= 0) & (there < n_z))
            def _():
                line_copy(j, z, way).wait_send()

        def inner(i, _):
            away = (i + 1) // 2
            way = 1 - 2 * lax.rem(i, 2)
            zz = z + way * away

            @pl.when((zz >= 0) & (zz < n_z))
            def _():
                onward = z - way

                @pl.when((onward >= 0) & (onward < n_z))
                def _():
                    line_copy(j, zz, -way).wait_send()

                pair_copy(j, zz, c).wait_send()

            return 0

        lax.fori_loop(1, 2 * n_z - 1, inner, 0)
        return 0

    lax.fori_loop(0, chunks, drain, 0)
    for seq in range(seqs):
        for peer in peers:
            tot_copy(seq, peer, sp).wait_send()
            term_copy(seq, peer, sp).wait_send()
            read_copy(seq, peer, sp).wait_send()


def per_device(
    n_sp,
    n_z,
    inputs,
    in_gain,
    key_weight,
    value_weight,
    decay_down,
    decay_up,
    decay_bias,
    new_query,
    out_gain,
):
    seqs, span, feats = inputs.shape
    model, key_cols = key_weight.shape
    value_cols = value_weight.shape[1]
    rank = decay_down.shape[1]
    heads = key_cols // DK
    chunks = seqs * (span // CHUNK)
    share = DK // n_sp
    vmem = pl.BlockSpec(memory_space=pltpu.VMEM)
    hbm = pl.BlockSpec(memory_space=pl.ANY)
    dma = pltpu.SemaphoreType.DMA
    return pl.pallas_call(
        functools.partial(kernel, n_sp, n_z),
        out_shape=(
            jax.ShapeDtypeStruct((seqs, heads, share, DV), BF16),
            jax.ShapeDtypeStruct((seqs, heads * DV), BF16),
        ),
        in_specs=[hbm, vmem, hbm, hbm, hbm, hbm, hbm, vmem, vmem],
        out_specs=(vmem, vmem),
        scratch_shapes=[
            pltpu.VMEM((chunks, n_z, 2, CHUNK, feats), BF16),
            pltpu.VMEM((model, key_cols), BF16),
            pltpu.VMEM((model, value_cols), BF16),
            pltpu.VMEM((model, rank), BF16),
            pltpu.VMEM((rank, key_cols), BF16),
            pltpu.VMEM((1, key_cols), F32),
            pltpu.VMEM((CHUNK, key_cols), F32),
            pltpu.VMEM((CHUNK, value_cols), F32),
            pltpu.VMEM((CHUNK, rank), F32),
            pltpu.VMEM((CHUNK, 128), F32),
            pltpu.VMEM((seqs, key_cols, DV), F32),
            pltpu.VMEM((1, key_cols), F32),
            pltpu.VMEM((seqs, n_sp, 1, key_cols), F32),
            pltpu.VMEM((seqs, n_sp, heads, share, DV), F32),
            pltpu.VMEM((seqs, n_sp, heads, share, DV), F32),
            pltpu.VMEM((seqs, n_sp, heads, DV), F32),
            dma((5,)),
            dma((chunks,)),
            dma((2, chunks, n_z)),
            dma((chunks, n_z)),
            dma((chunks, n_z, 2)),
            dma((seqs, n_sp)),
            dma((seqs, n_sp)),
            dma((seqs, n_sp)),
            dma((seqs, n_sp)),
            dma((seqs, n_sp)),
            dma((seqs, n_sp)),
        ],
        compiler_params=pltpu.CompilerParams(
            collective_id=0, has_side_effects=True, vmem_limit_bytes=60 * 1024 * 1024
        ),
    )(
        inputs,
        in_gain.reshape(2 * n_z, 1, feats),
        key_weight,
        value_weight,
        decay_down,
        decay_up,
        decay_bias.reshape(1, -1),
        new_query,
        out_gain.reshape(1, -1),
    )


def solution(mesh):
    in_specs = (
        P(None, "sp", "tp"),
        P(),
        P(None, "tp"),
        P(None, "tp"),
        P(),
        P(),
        P(),
        P(None, "tp"),
        P(),
    )
    out_specs = (P(None, "tp", "sp", None), P(None, "tp"))
    return jax.shard_map(
        functools.partial(per_device, mesh.shape["sp"], mesh.shape["tp"] // 2),
        mesh=mesh,
        in_specs=in_specs,
        out_specs=out_specs,
        check_vma=False,
    )
```

```python
import functools

import jax
import jax.numpy as jnp
from jax import lax
from jax.experimental import pallas as pl
from jax.experimental.pallas import tpu as pltpu
from jax.sharding import PartitionSpec as P

DK = 128
DV = 256
CHUNK = 128
AHEAD = 4
MESH = pl.DeviceIdType.MESH
F32 = jnp.float32
BF16 = jnp.bfloat16


def split3(value):
    high = value.astype(BF16)
    rest = value - high.astype(F32)
    middle = rest.astype(BF16)
    low = (rest - middle.astype(F32)).astype(BF16)
    return high, middle, low


def kernel(
    n_sp,
    n_z,
    x_ref,
    gain_ref,
    wk_hbm,
    wv_hbm,
    wd_hbm,
    up_hbm,
    bias_hbm,
    query_ref,
    cache_ref,
    parts_ref,
    xbuf,
    wk,
    wv,
    wd,
    up,
    bias,
    acc_k,
    acc_v,
    acc_l,
    acc_s,
    state,
    carry,
    tots,
    terms,
    landed,
    reads,
    load_sem,
    own_sem,
    line_send,
    pair_send,
    recv,
    tot_send,
    tot_recv,
    term_send,
    term_recv,
    read_send,
    read_recv,
):
    seqs, span, feats = x_ref.shape
    per_seq = span // CHUNK
    chunks = seqs * per_seq
    heads = wk_hbm.shape[1] // DK
    share = DK // n_sp
    model = n_z * 2 * feats
    sp = lax.axis_index("sp")
    tp = lax.axis_index("tp")
    z = tp // 2
    c = lax.rem(tp, 2)
    key_cols = heads * DK

    first = pl.multiple_of(tp * key_cols, key_cols)
    loads = [
        pltpu.make_async_copy(wk_hbm, wk, load_sem.at[0]),
        pltpu.make_async_copy(wv_hbm, wv, load_sem.at[1]),
        pltpu.make_async_copy(wd_hbm, wd, load_sem.at[2]),
        pltpu.make_async_copy(up_hbm.at[:, pl.ds(first, key_cols)], up, load_sem.at[3]),
        pltpu.make_async_copy(bias_hbm.at[:, pl.ds(first, key_cols)], bias, load_sem.at[4]),
    ]

    def chunk_rows(j):
        seq = j // per_seq
        start = (per_seq - 1 - lax.rem(j, per_seq)) * CHUNK
        return seq, pl.multiple_of(start, CHUNK)

    def own_copy(j):
        seq, start = chunk_rows(j)
        return pltpu.make_async_copy(
            x_ref.at[seq, pl.ds(start, CHUNK), :], xbuf.at[j, z, c], own_sem.at[j]
        )

    def line_copy(j, zz, way):
        return pltpu.make_async_remote_copy(
            src_ref=xbuf.at[j, zz, c],
            dst_ref=xbuf.at[j, zz, c],
            send_sem=line_send.at[(way + 1) // 2, j, zz],
            recv_sem=recv.at[j, zz, c],
            device_id={"tp": tp + 2 * way},
            device_id_type=MESH,
        )

    def pair_copy(j, zz, cc):
        return pltpu.make_async_remote_copy(
            src_ref=xbuf.at[j, zz, cc],
            dst_ref=xbuf.at[j, zz, cc],
            send_sem=pair_send.at[j, zz],
            recv_sem=recv.at[j, zz, cc],
            device_id={"tp": tp + 1 - 2 * c},
            device_id_type=MESH,
        )

    for j in range(chunks):
        own_copy(j).start()

    barrier = pltpu.get_barrier_semaphore()
    for way in (-1, 1):
        there = z + way

        @pl.when((there >= 0) & (there < n_z))
        def _():
            pl.semaphore_signal(
                barrier, inc=1, device_id={"tp": tp + 2 * way}, device_id_type=MESH
            )

    pl.semaphore_signal(barrier, inc=1, device_id={"tp": tp + 1 - 2 * c}, device_id_type=MESH)
    for off in range(1, n_sp):
        pl.semaphore_signal(
            barrier, inc=1, device_id={"sp": lax.rem(sp + off, n_sp)}, device_id_type=MESH
        )
    lines = jnp.where(z > 0, 1, 0) + jnp.where(z < n_z - 1, 1, 0)
    pl.semaphore_wait(barrier, lines + n_sp)

    def send_own(j):
        own_copy(j).wait()
        for way in (-1, 1):
            there = z + way

            @pl.when((there >= 0) & (there < n_z))
            def _():
                line_copy(j, z, way).start()

        pair_copy(j, z, c).start()

    for j in range(min(AHEAD, chunks)):
        send_own(j)
    for load in loads:
        load.start()
    for load in loads:
        load.wait()

    def clear_chunk():
        acc_k[...] = jnp.zeros_like(acc_k)
        acc_v[...] = jnp.zeros_like(acc_v)
        acc_l[...] = jnp.zeros_like(acc_l)
        acc_s[...] = jnp.zeros_like(acc_s)

    def add_shard(j, zz, cc):
        slot = zz * 2 + cc
        wide = xbuf[j, zz, cc].astype(F32)
        scaled = (wide * gain_ref[slot]).astype(BF16)
        rows = pl.ds(pl.multiple_of(slot * feats, feats), feats)
        acc_k[...] += jnp.dot(scaled, wk[rows, :], preferred_element_type=F32)
        acc_v[...] += jnp.dot(scaled, wv[rows, :], preferred_element_type=F32)
        acc_l[...] += lax.dot_general(
            scaled, wd[:, rows], (((1,), (1,)), ((), ())), preferred_element_type=F32
        )
        square = wide * wide
        total = square[:, 0:128]
        for lane in range(128, feats, 128):
            total = total + square[:, lane : lane + 128]
        acc_s[...] += total

    def gather_step(j, i):
        away = (i + 1) // 2
        way = 1 - 2 * lax.rem(i, 2)
        zz = z + way * away

        @pl.when((zz >= 0) & (zz < n_z))
        def _():
            @pl.when(i > 0)
            def _():
                line_copy(j, zz, 1).wait_recv()
                onward = z - way

                @pl.when((onward >= 0) & (onward < n_z))
                def _():
                    line_copy(j, zz, -way).start()

                pair_copy(j, zz, c).start()

            add_shard(j, zz, c)
            pair_copy(j, zz, 1 - c).wait_recv()
            add_shard(j, zz, 1 - c)

    def finish_chunk(j):
        seq = j // per_seq

        @pl.when(lax.rem(j, per_seq) == 0)
        def _():
            carry[...] = jnp.zeros_like(carry)
            state[seq] = jnp.zeros(state.shape[1:], F32)

        inv_rms = lax.rsqrt(jnp.sum(acc_s[...], axis=1, keepdims=True) / model + 1e-06)
        low_rank = acc_l[...] * inv_rms
        gate = (
            jnp.dot(
                low_rank,
                up[...].astype(F32),
                precision=lax.Precision.HIGHEST,
                preferred_element_type=F32,
            )
            + bias[...]
        )
        log_decay = (jnp.minimum(gate, 0.0) - jnp.log1p(jnp.exp(-jnp.abs(gate)))) / 16.0
        later = (
            lax.broadcasted_iota(jnp.int32, (CHUNK, CHUNK), 1)
            > lax.broadcasted_iota(jnp.int32, (CHUNK, CHUNK), 0)
        ).astype(BF16)
        suffix = carry[...]
        for piece in split3(log_decay):
            suffix = suffix + jnp.dot(later, piece, preferred_element_type=F32)
        carry[...] = carry[...] + jnp.sum(log_decay, axis=0, keepdims=True)
        last = lax.rem(j, per_seq) == per_seq - 1

        @pl.when(last)
        def _():
            send_total(seq)

        keys = (acc_k[...] * inv_rms).astype(BF16).astype(F32)
        weighted = keys * jnp.exp(suffix)
        values = (acc_v[...] * inv_rms).astype(BF16)
        for h in range(heads):
            part = weighted[:, h * DK : (h + 1) * DK].T.astype(BF16)
            rows = pl.ds(h * DK, DK)
            state[seq, rows, :] = state[seq, rows, :] + jnp.dot(
                part, values[:, h * DV : (h + 1) * DV], preferred_element_type=F32
            )

        @pl.when(last)
        def _():
            send_terms(seq)

    peers = [lax.rem(sp + off, n_sp) for off in range(1, n_sp)]

    def tot_copy(seq, peer, slot):
        return pltpu.make_async_remote_copy(
            src_ref=tots.at[seq, sp],
            dst_ref=tots.at[seq, slot],
            send_sem=tot_send.at[seq, peer],
            recv_sem=tot_recv.at[seq, slot],
            device_id={"sp": peer},
            device_id_type=MESH,
        )

    def term_copy(seq, peer, slot):
        return pltpu.make_async_remote_copy(
            src_ref=terms.at[seq, peer],
            dst_ref=landed.at[seq, slot],
            send_sem=term_send.at[seq, peer],
            recv_sem=term_recv.at[seq, slot],
            device_id={"sp": peer},
            device_id_type=MESH,
        )

    def read_copy(seq, peer, slot):
        return pltpu.make_async_remote_copy(
            src_ref=reads.at[seq, sp],
            dst_ref=reads.at[seq, slot],
            send_sem=read_send.at[seq, peer],
            recv_sem=read_recv.at[seq, slot],
            device_id={"sp": peer},
            device_id_type=MESH,
        )

    def send_total(seq):
        tots[seq, sp] = carry[...]
        for peer in peers:
            tot_copy(seq, peer, sp).start()

    def send_terms(seq):
        for h in range(heads):
            for p in range(n_sp):
                row = h * DK + p * share
                terms[seq, p, h] = state[seq, row : row + share, :].astype(BF16)
        for peer in peers:
            term_copy(seq, peer, sp).start()

    def send_reads(seq):
        chosen = (
            lax.broadcasted_iota(jnp.int32, (share, DK), 0) + sp * share
            == lax.broadcasted_iota(jnp.int32, (share, DK), 1)
        )

        def column(row):
            return jnp.sum(jnp.where(chosen, row, 0.0), axis=1, keepdims=True)

        for peer in peers:
            tot_copy(seq, peer, peer).wait_recv()
        after = jnp.zeros((1, key_cols), F32)
        factors = [None] * n_sp
        for p in reversed(range(n_sp)):
            decay = jnp.exp(after)
            factors[p] = [column(decay[:, h * DK : (h + 1) * DK]) for h in range(heads)]
            after = after + tots[seq, p]
        for peer in peers:
            term_copy(seq, peer, peer).wait_recv()
        own = [
            state[seq, pl.ds(pl.multiple_of(h * DK + sp * share, share), share), :]
            for h in range(heads)
        ]
        sums = []
        for h in range(heads):
            total = jnp.zeros((share, DV), F32)
            for p in range(n_sp):
                block = jnp.where(p == sp, own[h], landed[seq, p, h].astype(F32))
                total = total + factors[p][h] * block
            sums.append(total)
        for h in range(heads):
            cache = sums[h].astype(BF16)
            cache_ref[seq, h] = cache
            queries = query_ref[seq : seq + 1, h * DK : (h + 1) * DK].astype(F32)
            reads[seq, sp, h : h + 1, :] = jnp.sum(
                column(queries) * cache.astype(F32), axis=0, keepdims=True
            )
        for peer in peers:
            read_copy(seq, peer, sp).start()

    def give_read(seq):
        for peer in peers:
            read_copy(seq, peer, peer).wait_recv()
        parts_ref[seq] = reads[seq]

    def chunk_step(j, _):
        @pl.when(j + AHEAD < chunks)
        def _():
            send_own(j + AHEAD)

        clear_chunk()

        def inner(i, _):
            gather_step(j, i)
            return 0

        lax.fori_loop(0, 2 * n_z - 1, inner, 0)
        finish_chunk(j)
        return 0

    lax.fori_loop(0, chunks - 1, chunk_step, 0)
    for seq in range(seqs - 1):
        send_reads(seq)
    chunk_step(chunks - 1, 0)
    def drain(j, _):
        pair_copy(j, z, c).wait_send()
        for way in (-1, 1):
            there = z + way

            @pl.when((there >= 0) & (there < n_z))
            def _():
                line_copy(j, z, way).wait_send()

        def inner(i, _):
            away = (i + 1) // 2
            way = 1 - 2 * lax.rem(i, 2)
            zz = z + way * away

            @pl.when((zz >= 0) & (zz < n_z))
            def _():
                onward = z - way

                @pl.when((onward >= 0) & (onward < n_z))
                def _():
                    line_copy(j, zz, -way).wait_send()

                pair_copy(j, zz, c).wait_send()

            return 0

        lax.fori_loop(1, 2 * n_z - 1, inner, 0)
        return 0

    lax.fori_loop(0, chunks, drain, 0)
    send_reads(seqs - 1)
    for seq in range(seqs):
        give_read(seq)
    for seq in range(seqs):
        for peer in peers:
            tot_copy(seq, peer, sp).wait_send()
            term_copy(seq, peer, sp).wait_send()
            read_copy(seq, peer, sp).wait_send()


def norm_kernel(cache_in, parts_ref, gain_ref, cache_ref, read_ref):
    cache_ref[...] = cache_in[...]
    seqs, n_sp, heads, _ = parts_ref.shape
    for seq in range(seqs):
        readout = parts_ref[seq, 0]
        for p in range(1, n_sp):
            readout = readout + parts_ref[seq, p]
        mean = jnp.mean(readout * readout, axis=-1, keepdims=True)
        normed = (readout * lax.rsqrt(mean + 1e-06) * gain_ref[...]).astype(BF16)
        for h in range(heads):
            read_ref[seq : seq + 1, h * DV : (h + 1) * DV] = normed[h : h + 1, :]


def per_device(
    n_sp,
    n_z,
    inputs,
    in_gain,
    key_weight,
    value_weight,
    decay_down,
    decay_up,
    decay_bias,
    new_query,
    out_gain,
):
    seqs, span, feats = inputs.shape
    model, key_cols = key_weight.shape
    value_cols = value_weight.shape[1]
    rank = decay_down.shape[1]
    heads = key_cols // DK
    chunks = seqs * (span // CHUNK)
    share = DK // n_sp
    vmem = pl.BlockSpec(memory_space=pltpu.VMEM)
    hbm = pl.BlockSpec(memory_space=pl.ANY)
    dma = pltpu.SemaphoreType.DMA
    cache, parts = pl.pallas_call(
        functools.partial(kernel, n_sp, n_z),
        out_shape=(
            jax.ShapeDtypeStruct((seqs, heads, share, DV), BF16),
            jax.ShapeDtypeStruct((seqs, n_sp, heads, DV), F32),
        ),
        in_specs=[hbm, vmem, hbm, hbm, hbm, hbm, hbm, vmem],
        out_specs=(vmem, vmem),
        scratch_shapes=[
            pltpu.VMEM((chunks, n_z, 2, CHUNK, feats), BF16),
            pltpu.VMEM((model, key_cols), BF16),
            pltpu.VMEM((model, value_cols), BF16),
            pltpu.VMEM((rank, model), BF16),
            pltpu.VMEM((rank, key_cols), BF16),
            pltpu.VMEM((1, key_cols), F32),
            pltpu.VMEM((CHUNK, key_cols), F32),
            pltpu.VMEM((CHUNK, value_cols), F32),
            pltpu.VMEM((CHUNK, rank), F32),
            pltpu.VMEM((CHUNK, 128), F32),
            pltpu.VMEM((seqs, key_cols, DV), F32),
            pltpu.VMEM((1, key_cols), F32),
            pltpu.VMEM((seqs, n_sp, 1, key_cols), F32),
            pltpu.VMEM((seqs, n_sp, heads, share, DV), BF16),
            pltpu.VMEM((seqs, n_sp, heads, share, DV), BF16),
            pltpu.VMEM((seqs, n_sp, heads, DV), F32),
            dma((5,)),
            dma((chunks,)),
            dma((2, chunks, n_z)),
            dma((chunks, n_z)),
            dma((chunks, n_z, 2)),
            dma((seqs, n_sp)),
            dma((seqs, n_sp)),
            dma((seqs, n_sp)),
            dma((seqs, n_sp)),
            dma((seqs, n_sp)),
            dma((seqs, n_sp)),
        ],
        compiler_params=pltpu.CompilerParams(
            collective_id=0, has_side_effects=True, vmem_limit_bytes=60 * 1024 * 1024
        ),
    )(
        inputs,
        in_gain.reshape(2 * n_z, 1, feats),
        key_weight,
        value_weight,
        decay_down.T,
        decay_up,
        decay_bias.reshape(1, -1),
        new_query,
    )
    return pl.pallas_call(
        norm_kernel,
        out_shape=(
            jax.ShapeDtypeStruct((seqs, heads, share, DV), BF16),
            jax.ShapeDtypeStruct((seqs, heads * DV), BF16),
        ),
        in_specs=[vmem, vmem, vmem],
        out_specs=(vmem, vmem),
    )(cache, parts, out_gain.reshape(1, -1))


def solution(mesh):
    in_specs = (
        P(None, "sp", "tp"),
        P(),
        P(None, "tp"),
        P(None, "tp"),
        P(),
        P(),
        P(),
        P(None, "tp"),
        P(),
    )
    out_specs = (P(None, "tp", "sp", None), P(None, "tp"))
    return jax.shard_map(
        functools.partial(per_device, mesh.shape["sp"], mesh.shape["tp"] // 2),
        mesh=mesh,
        in_specs=in_specs,
        out_specs=out_specs,
        check_vma=False,
    )
```

```python
import functools

import jax
import jax.numpy as jnp
from jax import lax
from jax.experimental import pallas as pl
from jax.experimental.pallas import tpu as pltpu
from jax.sharding import PartitionSpec as P

DK = 128
DV = 256
CHUNK = 256
AHEAD = 2
MESH = pl.DeviceIdType.MESH
F32 = jnp.float32
BF16 = jnp.bfloat16


def split3(value):
    high = value.astype(BF16)
    rest = value - high.astype(F32)
    middle = rest.astype(BF16)
    low = (rest - middle.astype(F32)).astype(BF16)
    return high, middle, low


def kernel(
    n_sp,
    n_z,
    x_ref,
    gain_hbm,
    wk_hbm,
    wv_hbm,
    wd_hbm,
    up_hbm,
    bias_hbm,
    query_hbm,
    cache_ref,
    parts_ref,
    xbuf,
    wk,
    wv,
    wd,
    up,
    bias,
    gain_ref,
    query_ref,
    acc_k,
    acc_v,
    acc_l,
    acc_s,
    state,
    carry,
    tots,
    terms,
    landed,
    reads,
    load_sem,
    own_sem,
    line_send,
    relay_send,
    pair_send,
    recv,
    tot_send,
    tot_recv,
    term_send,
    term_recv,
    read_send,
    read_recv,
):
    seqs, span, feats = x_ref.shape
    per_seq = span // CHUNK
    chunks = seqs * per_seq
    heads = wk_hbm.shape[1] // DK
    share = DK // n_sp
    model = n_z * 2 * feats
    sp = lax.axis_index("sp")
    tp = lax.axis_index("tp")
    z = tp // 2
    c = lax.rem(tp, 2)
    key_cols = heads * DK

    first = pl.multiple_of(tp * key_cols, key_cols)
    loads = [
        pltpu.make_async_copy(wk_hbm, wk, load_sem.at[0]),
        pltpu.make_async_copy(wv_hbm, wv, load_sem.at[1]),
        pltpu.make_async_copy(wd_hbm, wd, load_sem.at[2]),
        pltpu.make_async_copy(up_hbm.at[:, pl.ds(first, key_cols)], up, load_sem.at[3]),
        pltpu.make_async_copy(bias_hbm.at[:, pl.ds(first, key_cols)], bias, load_sem.at[4]),
        pltpu.make_async_copy(gain_hbm, gain_ref, load_sem.at[5]),
        pltpu.make_async_copy(query_hbm, query_ref, load_sem.at[6]),
    ]

    def chunk_rows(j):
        seq = j // per_seq
        start = (per_seq - 1 - lax.rem(j, per_seq)) * CHUNK
        return seq, pl.multiple_of(start, CHUNK)

    def own_copy(j):
        seq, start = chunk_rows(j)
        return pltpu.make_async_copy(
            x_ref.at[seq, pl.ds(start, CHUNK), :], xbuf.at[j, z, c], own_sem.at[j]
        )

    def line_copy(j, there):
        return pltpu.make_async_remote_copy(
            src_ref=xbuf.at[j, z, c],
            dst_ref=xbuf.at[j, z, c],
            send_sem=line_send.at[j, there],
            recv_sem=recv.at[j, z, c],
            device_id={"tp": there * 2 + c},
            device_id_type=MESH,
        )

    def relay_copy(j, zz, end):
        return pltpu.make_async_remote_copy(
            src_ref=xbuf.at[j, zz, c],
            dst_ref=xbuf.at[j, zz, c],
            send_sem=relay_send.at[j, zz],
            recv_sem=recv.at[j, zz, c],
            device_id={"tp": end * 2 + c},
            device_id_type=MESH,
        )

    ends = ((0, 1), (n_z - 1, n_z - 2))

    def each_end(act):
        for end, inner in ends:

            @pl.when(z == inner)
            def _():
                act(end)

    def each_inner(act):
        for there in range(1, n_z - 1):

            @pl.when(z != there)
            def _():
                act(there)

    def each_relayed(zz, act):
        for end, inner in ends:
            beyond = zz > inner if end == 0 else zz < inner

            @pl.when((z == inner) & beyond)
            def _():
                act(end)

    def pair_copy(j, zz, cc):
        return pltpu.make_async_remote_copy(
            src_ref=xbuf.at[j, zz, cc],
            dst_ref=xbuf.at[j, zz, cc],
            send_sem=pair_send.at[j, zz],
            recv_sem=recv.at[j, zz, cc],
            device_id={"tp": tp + 1 - 2 * c},
            device_id_type=MESH,
        )

    for j in range(chunks):
        own_copy(j).start()
    for load in loads:
        load.start()

    barrier = pltpu.get_barrier_semaphore()
    at_end = (z == 0) | (z == n_z - 1)
    for there in range(n_z):
        met = z != there
        if n_z > 2 and there in (0, n_z - 1):
            met = met & jnp.logical_not(at_end)

        @pl.when(met)
        def _():
            pl.semaphore_signal(
                barrier, inc=1, device_id={"tp": there * 2 + c}, device_id_type=MESH
            )

    pl.semaphore_signal(barrier, inc=1, device_id={"tp": tp + 1 - 2 * c}, device_id_type=MESH)
    for off in range(1, n_sp):
        pl.semaphore_signal(
            barrier, inc=1, device_id={"sp": lax.rem(sp + off, n_sp)}, device_id_type=MESH
        )
    far = jnp.where(at_end, 1, 0) if n_z > 2 else 0
    pl.semaphore_wait(barrier, n_z - 1 + n_sp - far)

    def send_end(j):
        each_end(lambda end: line_copy(j, end).start())

    for j in range(chunks):
        own_copy(j).wait()
        each_inner(lambda there: line_copy(j, there).start())
        if j < AHEAD:
            send_end(j)
        pair_copy(j, z, c).start()
    for load in loads:
        load.wait()

    def clear_chunk():
        acc_k[...] = jnp.zeros_like(acc_k)
        acc_v[...] = jnp.zeros_like(acc_v)
        acc_l[...] = jnp.zeros_like(acc_l)
        acc_s[...] = jnp.zeros_like(acc_s)

    def add_shard(j, zz, cc):
        slot = zz * 2 + cc
        wide = xbuf[j, zz, cc].astype(F32)
        scaled = (wide * gain_ref[slot]).astype(BF16)
        rows = pl.ds(pl.multiple_of(slot * feats, feats), feats)
        acc_k[...] += jnp.dot(scaled, wk[rows, :], preferred_element_type=F32)
        acc_v[...] += jnp.dot(scaled, wv[rows, :], preferred_element_type=F32)
        acc_l[...] += lax.dot_general(
            scaled, wd[:, rows], (((1,), (1,)), ((), ())), preferred_element_type=F32
        )
        square = wide * wide
        total = square[:, 0:128]
        for lane in range(128, feats, 128):
            total = total + square[:, lane : lane + 128]
        acc_s[...] += total

    def gather_step(j, i):
        away = (i + 1) // 2
        way = 1 - 2 * lax.rem(i, 2)
        zz = z + way * away

        @pl.when((zz >= 0) & (zz < n_z))
        def _():
            @pl.when(i > 0)
            def _():
                relay_copy(j, zz, 0).wait_recv()
                each_relayed(zz, lambda end: relay_copy(j, zz, end).start())
                pair_copy(j, zz, c).start()

            add_shard(j, zz, c)
            pair_copy(j, zz, 1 - c).wait_recv()
            add_shard(j, zz, 1 - c)

    def finish_chunk(j):
        seq = j // per_seq

        @pl.when(lax.rem(j, per_seq) == 0)
        def _():
            carry[...] = jnp.zeros_like(carry)
            state[seq] = jnp.zeros(state.shape[1:], F32)

        inv_rms = lax.rsqrt(jnp.sum(acc_s[...], axis=1, keepdims=True) / model + 1e-06)
        low_rank = acc_l[...] * inv_rms
        gate = (
            jnp.dot(
                low_rank,
                up[...].astype(F32),
                precision=lax.Precision.HIGHEST,
                preferred_element_type=F32,
            )
            + bias[...]
        )
        log_decay = (jnp.minimum(gate, 0.0) - jnp.log1p(jnp.exp(-jnp.abs(gate)))) / 16.0
        later = (
            lax.broadcasted_iota(jnp.int32, (CHUNK, CHUNK), 1)
            > lax.broadcasted_iota(jnp.int32, (CHUNK, CHUNK), 0)
        ).astype(BF16)
        suffix = carry[...]
        for piece in split3(log_decay):
            suffix = suffix + jnp.dot(later, piece, preferred_element_type=F32)
        carry[...] = carry[...] + jnp.sum(log_decay, axis=0, keepdims=True)
        last = lax.rem(j, per_seq) == per_seq - 1

        @pl.when(last)
        def _():
            send_total(seq)

        keys = (acc_k[...] * inv_rms).astype(BF16).astype(F32)
        weighted = keys * jnp.exp(suffix)
        values = (acc_v[...] * inv_rms).astype(BF16)
        for h in range(heads):
            part = weighted[:, h * DK : (h + 1) * DK].T.astype(BF16)
            rows = pl.ds(h * DK, DK)
            state[seq, rows, :] = state[seq, rows, :] + jnp.dot(
                part, values[:, h * DV : (h + 1) * DV], preferred_element_type=F32
            )

        @pl.when(last)
        def _():
            send_terms(seq)

    peers = [lax.rem(sp + off, n_sp) for off in range(1, n_sp)]

    def tot_copy(seq, peer, slot):
        return pltpu.make_async_remote_copy(
            src_ref=tots.at[seq, sp],
            dst_ref=tots.at[seq, slot],
            send_sem=tot_send.at[seq, peer],
            recv_sem=tot_recv.at[seq, slot],
            device_id={"sp": peer},
            device_id_type=MESH,
        )

    def term_copy(seq, peer, slot):
        return pltpu.make_async_remote_copy(
            src_ref=terms.at[seq, peer],
            dst_ref=landed.at[seq, slot],
            send_sem=term_send.at[seq, peer],
            recv_sem=term_recv.at[seq, slot],
            device_id={"sp": peer},
            device_id_type=MESH,
        )

    def read_copy(seq, peer, slot):
        return pltpu.make_async_remote_copy(
            src_ref=reads.at[seq, sp],
            dst_ref=reads.at[seq, slot],
            send_sem=read_send.at[seq, peer],
            recv_sem=read_recv.at[seq, slot],
            device_id={"sp": peer},
            device_id_type=MESH,
        )

    def send_total(seq):
        tots[seq, sp] = carry[...]
        for peer in peers:
            tot_copy(seq, peer, sp).start()

    def send_terms(seq):
        for h in range(heads):
            for p in range(n_sp):
                row = h * DK + p * share
                terms[seq, p, h] = state[seq, row : row + share, :].astype(BF16)
        for peer in peers:
            term_copy(seq, peer, sp).start()

    def send_reads(seq):
        chosen = (
            lax.broadcasted_iota(jnp.int32, (share, DK), 0) + sp * share
            == lax.broadcasted_iota(jnp.int32, (share, DK), 1)
        )

        def column(row):
            return jnp.sum(jnp.where(chosen, row, 0.0), axis=1, keepdims=True)

        for peer in peers:
            tot_copy(seq, peer, peer).wait_recv()
        after = jnp.zeros((1, key_cols), F32)
        factors = [None] * n_sp
        for p in reversed(range(n_sp)):
            decay = jnp.exp(after)
            factors[p] = [column(decay[:, h * DK : (h + 1) * DK]) for h in range(heads)]
            after = after + tots[seq, p]
        for peer in peers:
            term_copy(seq, peer, peer).wait_recv()
        own = [
            state[seq, pl.ds(pl.multiple_of(h * DK + sp * share, share), share), :]
            for h in range(heads)
        ]
        sums = []
        for h in range(heads):
            total = jnp.zeros((share, DV), F32)
            for p in range(n_sp):
                block = jnp.where(p == sp, own[h], landed[seq, p, h].astype(F32))
                total = total + factors[p][h] * block
            sums.append(total)
        for h in range(heads):
            cache = sums[h].astype(BF16)
            cache_ref[seq, h] = cache
            queries = query_ref[seq : seq + 1, h * DK : (h + 1) * DK].astype(F32)
            reads[seq, sp, h : h + 1, :] = jnp.sum(
                column(queries) * cache.astype(F32), axis=0, keepdims=True
            )
        for peer in peers:
            read_copy(seq, peer, sp).start()

    def give_read(seq):
        for peer in peers:
            read_copy(seq, peer, peer).wait_recv()
        parts_ref[seq] = reads[seq]

    def drain(j, _):
        pair_copy(j, z, c).wait_send()
        each_inner(lambda there: line_copy(j, there).wait_send())
        each_end(lambda end: line_copy(j, end).wait_send())

        def inner(i, _):
            away = (i + 1) // 2
            way = 1 - 2 * lax.rem(i, 2)
            zz = z + way * away

            @pl.when((zz >= 0) & (zz < n_z))
            def _():
                each_relayed(zz, lambda end: relay_copy(j, zz, end).wait_send())
                pair_copy(j, zz, c).wait_send()

            return 0

        lax.fori_loop(1, 2 * n_z - 1, inner, 0)
        return 0

    def chunk_step(j, _):
        @pl.when(j + AHEAD < chunks)
        def _():
            send_end(j + AHEAD)

        clear_chunk()

        def inner(i, _):
            gather_step(j, i)
            return 0

        lax.fori_loop(0, 2 * n_z - 1, inner, 0)
        finish_chunk(j)

        @pl.when((j > 0) & (j < chunks - 1))
        def _():
            drain(j - 1, 0)

        return 0

    lax.fori_loop(0, chunks - 1, chunk_step, 0)
    for seq in range(seqs - 1):
        send_reads(seq)
    chunk_step(chunks - 1, 0)
    if chunks > 1:
        drain(chunks - 2, 0)
    drain(chunks - 1, 0)
    send_reads(seqs - 1)
    for seq in range(seqs):
        give_read(seq)
    for seq in range(seqs):
        for peer in peers:
            tot_copy(seq, peer, sp).wait_send()
            term_copy(seq, peer, sp).wait_send()
            read_copy(seq, peer, sp).wait_send()


def norm_kernel(cache_in, parts_ref, gain_ref, cache_ref, read_ref):
    cache_ref[...] = cache_in[...]
    seqs, n_sp, heads, _ = parts_ref.shape
    for seq in range(seqs):
        readout = parts_ref[seq, 0]
        for p in range(1, n_sp):
            readout = readout + parts_ref[seq, p]
        mean = jnp.mean(readout * readout, axis=-1, keepdims=True)
        normed = (readout * lax.rsqrt(mean + 1e-06) * gain_ref[...]).astype(BF16)
        for h in range(heads):
            read_ref[seq : seq + 1, h * DV : (h + 1) * DV] = normed[h : h + 1, :]


def per_device(
    n_sp,
    n_z,
    inputs,
    in_gain,
    key_weight,
    value_weight,
    decay_down,
    decay_up,
    decay_bias,
    new_query,
    out_gain,
):
    seqs, span, feats = inputs.shape
    model, key_cols = key_weight.shape
    value_cols = value_weight.shape[1]
    rank = decay_down.shape[1]
    heads = key_cols // DK
    chunks = seqs * (span // CHUNK)
    share = DK // n_sp
    vmem = pl.BlockSpec(memory_space=pltpu.VMEM)
    hbm = pl.BlockSpec(memory_space=pl.ANY)
    dma = pltpu.SemaphoreType.DMA
    cache, parts = pl.pallas_call(
        functools.partial(kernel, n_sp, n_z),
        out_shape=(
            jax.ShapeDtypeStruct((seqs, heads, share, DV), BF16),
            jax.ShapeDtypeStruct((seqs, n_sp, heads, DV), F32),
        ),
        in_specs=[hbm] * 8,
        out_specs=(vmem, vmem),
        scratch_shapes=[
            pltpu.VMEM((chunks, n_z, 2, CHUNK, feats), BF16),
            pltpu.VMEM((model, key_cols), BF16),
            pltpu.VMEM((model, value_cols), BF16),
            pltpu.VMEM((rank, model), BF16),
            pltpu.VMEM((rank, key_cols), BF16),
            pltpu.VMEM((1, key_cols), F32),
            pltpu.VMEM((2 * n_z, 1, feats), F32),
            pltpu.VMEM((seqs, key_cols), BF16),
            pltpu.VMEM((CHUNK, key_cols), F32),
            pltpu.VMEM((CHUNK, value_cols), F32),
            pltpu.VMEM((CHUNK, rank), F32),
            pltpu.VMEM((CHUNK, 128), F32),
            pltpu.VMEM((seqs, key_cols, DV), F32),
            pltpu.VMEM((1, key_cols), F32),
            pltpu.VMEM((seqs, n_sp, 1, key_cols), F32),
            pltpu.VMEM((seqs, n_sp, heads, share, DV), BF16),
            pltpu.VMEM((seqs, n_sp, heads, share, DV), BF16),
            pltpu.VMEM((seqs, n_sp, heads, DV), F32),
            dma((7,)),
            dma((chunks,)),
            dma((chunks, n_z)),
            dma((chunks, n_z)),
            dma((chunks, n_z)),
            dma((chunks, n_z, 2)),
            dma((seqs, n_sp)),
            dma((seqs, n_sp)),
            dma((seqs, n_sp)),
            dma((seqs, n_sp)),
            dma((seqs, n_sp)),
            dma((seqs, n_sp)),
        ],
        compiler_params=pltpu.CompilerParams(
            collective_id=0, has_side_effects=True, vmem_limit_bytes=60 * 1024 * 1024
        ),
    )(
        inputs,
        in_gain.reshape(2 * n_z, 1, feats),
        key_weight,
        value_weight,
        decay_down.T,
        decay_up,
        decay_bias.reshape(1, -1),
        new_query,
    )
    return pl.pallas_call(
        norm_kernel,
        out_shape=(
            jax.ShapeDtypeStruct((seqs, heads, share, DV), BF16),
            jax.ShapeDtypeStruct((seqs, heads * DV), BF16),
        ),
        in_specs=[vmem, vmem, vmem],
        out_specs=(vmem, vmem),
    )(cache, parts, out_gain.reshape(1, -1))


def solution(mesh):
    in_specs = (
        P(None, "sp", "tp"),
        P(),
        P(None, "tp"),
        P(None, "tp"),
        P(),
        P(),
        P(),
        P(None, "tp"),
        P(),
    )
    out_specs = (P(None, "tp", "sp", None), P(None, "tp"))
    return jax.shard_map(
        functools.partial(per_device, mesh.shape["sp"], mesh.shape["tp"] // 2),
        mesh=mesh,
        in_specs=in_specs,
        out_specs=out_specs,
        check_vma=False,
    )
```

```python
import functools

import jax
import jax.numpy as jnp
from jax import lax
from jax.experimental import pallas as pl
from jax.experimental.pallas import tpu as pltpu
from jax.sharding import PartitionSpec as P

DK = 128
DV = 256
CHUNK = 256
AHEAD = 2
MESH = pl.DeviceIdType.MESH
F32 = jnp.float32
BF16 = jnp.bfloat16


def split3(value):
    high = value.astype(BF16)
    rest = value - high.astype(F32)
    middle = rest.astype(BF16)
    low = (rest - middle.astype(F32)).astype(BF16)
    return high, middle, low


def kernel(
    n_sp,
    n_z,
    x_ref,
    gain_hbm,
    wk_hbm,
    wv_hbm,
    wd_hbm,
    up_hbm,
    bias_hbm,
    query_hbm,
    cache_ref,
    parts_ref,
    xbuf,
    wk,
    wv,
    wd,
    up,
    bias,
    gain_ref,
    query_ref,
    acc_k,
    acc_v,
    acc_l,
    acc_s,
    state,
    carry,
    tots,
    terms,
    landed,
    reads,
    load_sem,
    own_sem,
    line_send,
    relay_send,
    pair_send,
    recv,
    tot_send,
    tot_recv,
    term_send,
    term_recv,
    read_send,
    read_recv,
):
    seqs, span, feats = x_ref.shape
    per_seq = span // CHUNK
    chunks = seqs * per_seq
    heads = wk_hbm.shape[1] // DK
    share = DK // n_sp
    model = n_z * 2 * feats
    sp = lax.axis_index("sp")
    tp = lax.axis_index("tp")
    z = tp // 2
    c = lax.rem(tp, 2)
    key_cols = heads * DK

    first = pl.multiple_of(tp * key_cols, key_cols)
    loads = [
        pltpu.make_async_copy(wk_hbm, wk, load_sem.at[0]),
        pltpu.make_async_copy(wv_hbm, wv, load_sem.at[1]),
        pltpu.make_async_copy(wd_hbm, wd, load_sem.at[2]),
        pltpu.make_async_copy(up_hbm.at[:, pl.ds(first, key_cols)], up, load_sem.at[3]),
        pltpu.make_async_copy(bias_hbm.at[:, pl.ds(first, key_cols)], bias, load_sem.at[4]),
        pltpu.make_async_copy(gain_hbm, gain_ref, load_sem.at[5]),
        pltpu.make_async_copy(query_hbm, query_ref, load_sem.at[6]),
    ]

    def chunk_rows(j):
        seq = j // per_seq
        start = (per_seq - 1 - lax.rem(j, per_seq)) * CHUNK
        return seq, pl.multiple_of(start, CHUNK)

    def own_copy(j):
        seq, start = chunk_rows(j)
        return pltpu.make_async_copy(
            x_ref.at[seq, pl.ds(start, CHUNK), :], xbuf.at[j, z, c], own_sem.at[j]
        )

    def line_copy(j, there):
        return pltpu.make_async_remote_copy(
            src_ref=xbuf.at[j, z, c],
            dst_ref=xbuf.at[j, z, c],
            send_sem=line_send.at[j, there],
            recv_sem=recv.at[j, z, c],
            device_id={"tp": there * 2 + c},
            device_id_type=MESH,
        )

    def relay_copy(j, zz, end):
        return pltpu.make_async_remote_copy(
            src_ref=xbuf.at[j, zz, c],
            dst_ref=xbuf.at[j, zz, c],
            send_sem=relay_send.at[j, zz],
            recv_sem=recv.at[j, zz, c],
            device_id={"tp": end * 2 + c},
            device_id_type=MESH,
        )

    ends = ((0, 1), (n_z - 1, n_z - 2))

    def each_end(act):
        for end, inner in ends:

            @pl.when(z == inner)
            def _():
                act(end)

    def each_inner(act):
        for there in range(1, n_z - 1):

            @pl.when(z != there)
            def _():
                act(there)

    def each_relayed(zz, act):
        for end, inner in ends:
            beyond = zz > inner if end == 0 else zz < inner

            @pl.when((z == inner) & beyond)
            def _():
                act(end)

    def pair_copy(j, zz, cc):
        return pltpu.make_async_remote_copy(
            src_ref=xbuf.at[j, zz, cc],
            dst_ref=xbuf.at[j, zz, cc],
            send_sem=pair_send.at[j, zz],
            recv_sem=recv.at[j, zz, cc],
            device_id={"tp": tp + 1 - 2 * c},
            device_id_type=MESH,
        )

    for j in range(chunks):
        own_copy(j).start()
    for load in loads:
        load.start()

    barrier = pltpu.get_barrier_semaphore()
    at_end = (z == 0) | (z == n_z - 1)
    for there in range(n_z):
        met = z != there
        if n_z > 2 and there in (0, n_z - 1):
            met = met & jnp.logical_not(at_end)

        @pl.when(met)
        def _():
            pl.semaphore_signal(
                barrier, inc=1, device_id={"tp": there * 2 + c}, device_id_type=MESH
            )

    pl.semaphore_signal(barrier, inc=1, device_id={"tp": tp + 1 - 2 * c}, device_id_type=MESH)
    for off in range(1, n_sp):
        pl.semaphore_signal(
            barrier, inc=1, device_id={"sp": lax.rem(sp + off, n_sp)}, device_id_type=MESH
        )
    far = jnp.where(at_end, 1, 0) if n_z > 2 else 0
    pl.semaphore_wait(barrier, n_z - 1 + n_sp - far)

    def send_end(j):
        each_end(lambda end: line_copy(j, end).start())

    for j in range(chunks):
        own_copy(j).wait()
        each_inner(lambda there: line_copy(j, there).start())
        if j < AHEAD:
            send_end(j)
        pair_copy(j, z, c).start()
    for load in loads:
        load.wait()

    def clear_chunk():
        acc_k[...] = jnp.zeros_like(acc_k)
        acc_v[...] = jnp.zeros_like(acc_v)
        acc_l[...] = jnp.zeros_like(acc_l)
        acc_s[...] = jnp.zeros_like(acc_s)

    def add_shard(j, zz, cc):
        slot = zz * 2 + cc
        wide = xbuf[j, zz, cc].astype(F32)
        scaled = (wide * gain_ref[slot]).astype(BF16)
        rows = pl.ds(pl.multiple_of(slot * feats, feats), feats)
        acc_k[...] += jnp.dot(scaled, wk[rows, :], preferred_element_type=F32)
        acc_v[...] += jnp.dot(scaled, wv[rows, :], preferred_element_type=F32)
        acc_l[...] += lax.dot_general(
            scaled, wd[:, rows], (((1,), (1,)), ((), ())), preferred_element_type=F32
        )
        square = wide * wide
        total = square[:, 0:128]
        for lane in range(128, feats, 128):
            total = total + square[:, lane : lane + 128]
        acc_s[...] += total

    def gather_step(j, i):
        away = (i + 1) // 2
        way = 1 - 2 * lax.rem(i, 2)
        zz = z + way * away

        @pl.when((zz >= 0) & (zz < n_z))
        def _():
            @pl.when(i > 0)
            def _():
                relay_copy(j, zz, 0).wait_recv()
                each_relayed(zz, lambda end: relay_copy(j, zz, end).start())
                pair_copy(j, zz, c).start()

            add_shard(j, zz, c)
            pair_copy(j, zz, 1 - c).wait_recv()
            add_shard(j, zz, 1 - c)

    def finish_chunk(j):
        seq = j // per_seq

        @pl.when(lax.rem(j, per_seq) == 0)
        def _():
            carry[...] = jnp.zeros_like(carry)
            state[seq] = jnp.zeros(state.shape[1:], F32)

        inv_rms = lax.rsqrt(jnp.sum(acc_s[...], axis=1, keepdims=True) / model + 1e-06)
        low_rank = acc_l[...] * inv_rms
        gate = bias[...] + jnp.dot(
            jnp.concatenate(split3(low_rank), axis=1),
            jnp.concatenate([up[...]] * 3, axis=0),
            preferred_element_type=F32,
        )
        log_decay = (jnp.minimum(gate, 0.0) - jnp.log1p(jnp.exp(-jnp.abs(gate)))) / 16.0
        later = (
            lax.broadcasted_iota(jnp.int32, (CHUNK, CHUNK), 1)
            > lax.broadcasted_iota(jnp.int32, (CHUNK, CHUNK), 0)
        ).astype(BF16)
        suffix = carry[...] + jnp.dot(
            jnp.concatenate([later] * 3, axis=1),
            jnp.concatenate(split3(log_decay), axis=0),
            preferred_element_type=F32,
        )
        carry[...] = carry[...] + jnp.sum(log_decay, axis=0, keepdims=True)
        last = lax.rem(j, per_seq) == per_seq - 1

        @pl.when(last)
        def _():
            send_total(seq)

        keys = (acc_k[...] * inv_rms).astype(BF16).astype(F32)
        weighted = keys * jnp.exp(suffix)
        values = (acc_v[...] * inv_rms).astype(BF16)
        for h in range(heads):
            part = weighted[:, h * DK : (h + 1) * DK].T.astype(BF16)
            rows = pl.ds(h * DK, DK)
            state[seq, rows, :] = state[seq, rows, :] + jnp.dot(
                part, values[:, h * DV : (h + 1) * DV], preferred_element_type=F32
            )

        @pl.when(last)
        def _():
            send_terms(seq)

    peers = [lax.rem(sp + off, n_sp) for off in range(1, n_sp)]

    def tot_copy(seq, peer, slot):
        return pltpu.make_async_remote_copy(
            src_ref=tots.at[seq, sp],
            dst_ref=tots.at[seq, slot],
            send_sem=tot_send.at[seq, peer],
            recv_sem=tot_recv.at[seq, slot],
            device_id={"sp": peer},
            device_id_type=MESH,
        )

    def term_copy(seq, peer, slot):
        return pltpu.make_async_remote_copy(
            src_ref=terms.at[seq, peer],
            dst_ref=landed.at[seq, slot],
            send_sem=term_send.at[seq, peer],
            recv_sem=term_recv.at[seq, slot],
            device_id={"sp": peer},
            device_id_type=MESH,
        )

    def read_copy(seq, peer, slot):
        return pltpu.make_async_remote_copy(
            src_ref=reads.at[seq, sp],
            dst_ref=reads.at[seq, slot],
            send_sem=read_send.at[seq, peer],
            recv_sem=read_recv.at[seq, slot],
            device_id={"sp": peer},
            device_id_type=MESH,
        )

    def send_total(seq):
        tots[seq, sp] = carry[...]
        for peer in peers:
            tot_copy(seq, peer, sp).start()

    def send_terms(seq):
        for h in range(heads):
            for p in range(n_sp):
                row = h * DK + p * share
                terms[seq, p, h] = state[seq, row : row + share, :].astype(BF16)
        for peer in peers:
            term_copy(seq, peer, sp).start()

    def send_reads(seq):
        chosen = (
            lax.broadcasted_iota(jnp.int32, (share, DK), 0) + sp * share
            == lax.broadcasted_iota(jnp.int32, (share, DK), 1)
        )

        def column(row):
            return jnp.sum(jnp.where(chosen, row, 0.0), axis=1, keepdims=True)

        for peer in peers:
            tot_copy(seq, peer, peer).wait_recv()
        after = jnp.zeros((1, key_cols), F32)
        factors = [None] * n_sp
        for p in reversed(range(n_sp)):
            decay = jnp.exp(after)
            factors[p] = [column(decay[:, h * DK : (h + 1) * DK]) for h in range(heads)]
            after = after + tots[seq, p]
        for peer in peers:
            term_copy(seq, peer, peer).wait_recv()
        own = [
            state[seq, pl.ds(pl.multiple_of(h * DK + sp * share, share), share), :]
            for h in range(heads)
        ]
        sums = []
        for h in range(heads):
            total = jnp.zeros((share, DV), F32)
            for p in range(n_sp):
                block = jnp.where(p == sp, own[h], landed[seq, p, h].astype(F32))
                total = total + factors[p][h] * block
            sums.append(total)
        for h in range(heads):
            cache = sums[h].astype(BF16)
            cache_ref[seq, h] = cache
            queries = query_ref[seq : seq + 1, h * DK : (h + 1) * DK].astype(F32)
            reads[seq, sp, h : h + 1, :] = jnp.sum(
                column(queries) * cache.astype(F32), axis=0, keepdims=True
            )
        for peer in peers:
            read_copy(seq, peer, sp).start()

    def give_read(seq):
        for peer in peers:
            read_copy(seq, peer, peer).wait_recv()
        parts_ref[seq] = reads[seq]

    def drain(j, _):
        pair_copy(j, z, c).wait_send()
        each_inner(lambda there: line_copy(j, there).wait_send())
        each_end(lambda end: line_copy(j, end).wait_send())

        def inner(i, _):
            away = (i + 1) // 2
            way = 1 - 2 * lax.rem(i, 2)
            zz = z + way * away

            @pl.when((zz >= 0) & (zz < n_z))
            def _():
                each_relayed(zz, lambda end: relay_copy(j, zz, end).wait_send())
                pair_copy(j, zz, c).wait_send()

            return 0

        lax.fori_loop(1, 2 * n_z - 1, inner, 0)
        return 0

    def chunk_step(j, _):
        @pl.when(j + AHEAD < chunks)
        def _():
            send_end(j + AHEAD)

        clear_chunk()

        def inner(i, _):
            gather_step(j, i)
            return 0

        lax.fori_loop(0, 2 * n_z - 1, inner, 0)
        finish_chunk(j)

        @pl.when((j > 0) & (j < chunks - 1))
        def _():
            drain(j - 1, 0)

        return 0

    lax.fori_loop(0, chunks - 1, chunk_step, 0)
    for seq in range(seqs - 1):
        send_reads(seq)
    chunk_step(chunks - 1, 0)
    if chunks > 1:
        drain(chunks - 2, 0)
    drain(chunks - 1, 0)
    send_reads(seqs - 1)
    for seq in range(seqs):
        give_read(seq)
    for seq in range(seqs):
        for peer in peers:
            tot_copy(seq, peer, sp).wait_send()
            term_copy(seq, peer, sp).wait_send()
            read_copy(seq, peer, sp).wait_send()


def norm_kernel(cache_in, parts_ref, gain_ref, cache_ref, read_ref):
    cache_ref[...] = cache_in[...]
    seqs, n_sp, heads, _ = parts_ref.shape
    for seq in range(seqs):
        readout = parts_ref[seq, 0]
        for p in range(1, n_sp):
            readout = readout + parts_ref[seq, p]
        mean = jnp.mean(readout * readout, axis=-1, keepdims=True)
        normed = (readout * lax.rsqrt(mean + 1e-06) * gain_ref[...]).astype(BF16)
        for h in range(heads):
            read_ref[seq : seq + 1, h * DV : (h + 1) * DV] = normed[h : h + 1, :]


def per_device(
    n_sp,
    n_z,
    inputs,
    in_gain,
    key_weight,
    value_weight,
    decay_down,
    decay_up,
    decay_bias,
    new_query,
    out_gain,
):
    seqs, span, feats = inputs.shape
    model, key_cols = key_weight.shape
    value_cols = value_weight.shape[1]
    rank = decay_down.shape[1]
    heads = key_cols // DK
    chunks = seqs * (span // CHUNK)
    share = DK // n_sp
    vmem = pl.BlockSpec(memory_space=pltpu.VMEM)
    hbm = pl.BlockSpec(memory_space=pl.ANY)
    dma = pltpu.SemaphoreType.DMA
    cache, parts = pl.pallas_call(
        functools.partial(kernel, n_sp, n_z),
        out_shape=(
            jax.ShapeDtypeStruct((seqs, heads, share, DV), BF16),
            jax.ShapeDtypeStruct((seqs, n_sp, heads, DV), F32),
        ),
        in_specs=[hbm] * 8,
        out_specs=(vmem, vmem),
        scratch_shapes=[
            pltpu.VMEM((chunks, n_z, 2, CHUNK, feats), BF16),
            pltpu.VMEM((model, key_cols), BF16),
            pltpu.VMEM((model, value_cols), BF16),
            pltpu.VMEM((rank, model), BF16),
            pltpu.VMEM((rank, key_cols), BF16),
            pltpu.VMEM((1, key_cols), F32),
            pltpu.VMEM((2 * n_z, 1, feats), F32),
            pltpu.VMEM((seqs, key_cols), BF16),
            pltpu.VMEM((CHUNK, key_cols), F32),
            pltpu.VMEM((CHUNK, value_cols), F32),
            pltpu.VMEM((CHUNK, rank), F32),
            pltpu.VMEM((CHUNK, 128), F32),
            pltpu.VMEM((seqs, key_cols, DV), F32),
            pltpu.VMEM((1, key_cols), F32),
            pltpu.VMEM((seqs, n_sp, 1, key_cols), F32),
            pltpu.VMEM((seqs, n_sp, heads, share, DV), BF16),
            pltpu.VMEM((seqs, n_sp, heads, share, DV), BF16),
            pltpu.VMEM((seqs, n_sp, heads, DV), F32),
            dma((7,)),
            dma((chunks,)),
            dma((chunks, n_z)),
            dma((chunks, n_z)),
            dma((chunks, n_z)),
            dma((chunks, n_z, 2)),
            dma((seqs, n_sp)),
            dma((seqs, n_sp)),
            dma((seqs, n_sp)),
            dma((seqs, n_sp)),
            dma((seqs, n_sp)),
            dma((seqs, n_sp)),
        ],
        compiler_params=pltpu.CompilerParams(
            collective_id=0, has_side_effects=True, vmem_limit_bytes=60 * 1024 * 1024
        ),
    )(
        inputs,
        in_gain.reshape(2 * n_z, 1, feats),
        key_weight,
        value_weight,
        decay_down.T,
        decay_up,
        decay_bias.reshape(1, -1),
        new_query,
    )
    return pl.pallas_call(
        norm_kernel,
        out_shape=(
            jax.ShapeDtypeStruct((seqs, heads, share, DV), BF16),
            jax.ShapeDtypeStruct((seqs, heads * DV), BF16),
        ),
        in_specs=[vmem, vmem, vmem],
        out_specs=(vmem, vmem),
    )(cache, parts, out_gain.reshape(1, -1))


def solution(mesh):
    in_specs = (
        P(None, "sp", "tp"),
        P(),
        P(None, "tp"),
        P(None, "tp"),
        P(),
        P(),
        P(),
        P(None, "tp"),
        P(),
    )
    out_specs = (P(None, "tp", "sp", None), P(None, "tp"))
    return jax.shard_map(
        functools.partial(per_device, mesh.shape["sp"], mesh.shape["tp"] // 2),
        mesh=mesh,
        in_specs=in_specs,
        out_specs=out_specs,
        check_vma=False,
    )
```
